32 devices in a mesh: sp: 8 (over z, x), tp: 4 (over y, core).
Axes of the slice: x: 2, y: 2, z: 4, core: 2. Of those that a mesh axis runs over, the one named last changes fastest.
Arguments:
- query_one: bfloat16 [2048, 512], P('sp', 'tp'), may hold values from -100 to 100, as said below
- key_one: bfloat16 [2048, 512], P('sp', 'tp'), may hold values from -8 to 8
- query_two: bfloat16 [2048, 512], P('sp', 'tp'), may hold values from -100 to 100, as said below
- key_two: bfloat16 [2048, 512], P('sp', 'tp'), may hold values from -8 to 8
- values: bfloat16 [2048, 1024], P('sp', 'tp'), may hold values from -6 to 6
- mix_lambda: float32 [8], P('tp'), may hold values from 0.3 to 0.8
- head_gain: float32 [128], replicated, may hold values from 0.1 to 1.9
- residual_in: bfloat16 [2048, 2048], P(('sp', 'tp')), may hold values from -6 to 6
- out_weight: bfloat16 [1024, 2048], replicated, may hold values from -0.1875 to 0.1875
- norm_gain: float32 [2048], replicated, may hold values from 0.1 to 1.9
- route_ids: int32 [2048, 2], P(('sp', 'tp')), may hold values from 0 to 15, all different within a row; in each aligned block of 64 rows (0 to 63, 64 to 127, ...) at most 16 rows name the same one
- route_logits: float32 [2048, 2], P(('sp', 'tp')), may hold values from -6 to 6
- group_prob: float32 [2048], P(('sp', 'tp')), may hold values from 0.25 to 1
- gate_weight: bfloat16 [16, 2048, 1024], P('sp', None, 'tp'), may hold values from -0.125 to 0.125
- up_weight: bfloat16 [16, 2048, 1024], P('sp', None, 'tp'), may hold values from -0.125 to 0.125
- down_weight: bfloat16 [16, 1024, 2048], P('sp', 'tp'), may hold values from -0.1875 to 0.1875
Outputs:
- layer_out: bfloat16 [2048, 2048], P(('sp', 'tp'))
The draws below stay inside these ranges and needn't reach their ends.
Inputs may be any that keep to these rules, and one draw needn't show every extreme that they name: `query_one`: drawn together with key_one. `query_two`: drawn together with key_two. `route_ids`: the experts of a row differ. In the rows of one device no expert is named more than 16 times, a bound that some block reaches.
All inputs are finite; a program needn't handle non-finite values.
Results may differ from the reference program's by a relative error of at most 0.014.
Values may be sent and summed in bfloat16 or wider, within the bound.
No kernel may reach another device: no remote copies, remote signals or barrier semaphores. Data moves between devices by JAX's collectives and lax.ppermute only.
A program may use at most 128 MiB of HBM per device.

```python
import math
import jax
import jax.numpy as jnp
import numpy as np
from jax import lax

D = 2048
HEADS = 8
QK = 64
VD = 128
FF = 1024
TOP = 2
ROWS = 64
TOKENS = 2048
MIXW = 1024
EXPERTS = 16
CAP = 16
N_SP = 8
N_TP = 4


def draw_maps(key, which):
    streams = jax.random.split(jax.random.fold_in(key, which), 2)
    keys_drawn = 1.3 * jax.random.normal(streams[0], (TOKENS, HEADS * QK), jnp.float32)
    queries = 1.3 * jax.random.normal(streams[1], (TOKENS, HEADS * QK), jnp.float32)
    queries = jnp.clip(queries, -100.0, 100.0)
    keys_drawn = jnp.clip(keys_drawn, -8.0, 8.0)
    return (queries, keys_drawn)


def draw_query_one(key, part):
    return draw_maps(key, 11)[0].astype(jnp.bfloat16)


def draw_key_one(key, part):
    return draw_maps(key, 11)[1].astype(jnp.bfloat16)


def draw_query_two(key, part):
    return draw_maps(key, 23)[0].astype(jnp.bfloat16)


def draw_key_two(key, part):
    return draw_maps(key, 23)[1].astype(jnp.bfloat16)


def levels(key, shape, cuts, low, top_value):
    loudness = 1.0
    for position, parts in cuts:
        steps = jax.random.uniform(jax.random.fold_in(jax.random.fold_in(key, 6), position), (parts,), jnp.float32, low / len(cuts), top_value / len(cuts))
        loudness = loudness * jnp.repeat(jnp.exp(steps), shape[position] // parts).reshape((-1,) + (1,) * (len(shape) - 1 - position))
    return loudness


def deal_out(stream_key, own, number, rows, count, top, most, slope):
    sequence = jax.random.permutation(stream_key, count)
    crowded, common = load_shares(count, rows * top, most, slope, True), load_shares(count, rows * top, most, slope, False)
    places = jnp.arange(count)

    def named(sizes, rotation):
        used = int((sizes > 0).sum())
        fixed = max(1, used // 4)
        passed = fixed + (places - fixed + rotation * (used - fixed)) % max(1, count - fixed)
        return jnp.zeros((count,), jnp.int32).at[sequence[jnp.where(places < fixed, places, passed)]].set(jnp.asarray(sizes, jnp.int32))

    sizes = jnp.where(number % 4 == 0, named(crowded, number // 4), named(common, number - number // 4 - 1))
    mixed = jax.random.permutation(jax.random.fold_in(own, 3), count)
    donor, taker = mixed[0:count // 2 * 2:2], mixed[1:count // 2 * 2:2]
    slack = jnp.minimum(sizes[donor] - 1, most - sizes[taker]) // 2
    slack = jnp.where((donor == sequence[0]) | (taker == sequence[0]) | (sizes[taker] == 0), 0, jnp.maximum(slack, 0))
    passed = jax.random.randint(jax.random.fold_in(own, 4), (count // 2,), 0, 1 << 20) % (slack + 1)
    sizes = sizes.at[donor].add(-passed).at[taker].add(passed)
    labels = jnp.searchsorted(jnp.cumsum(sizes), jnp.arange(rows * top), side="right").astype(jnp.int32)
    grid = labels.reshape(top, rows).T
    grid = grid[jax.random.permutation(jax.random.fold_in(own, 1), rows)]
    rotation = jax.random.randint(jax.random.fold_in(own, 2), (rows, 1), 0, top)
    return jnp.take_along_axis(grid, (jnp.arange(top)[None, :] + rotation) % top, axis=1)


def load_shares(count, total, most, lean, full):
    portions = [(1 << 20) // math.isqrt(rank ** lean) + 1 for rank in range(1, count + 1)]
    largest = most if full else min(most, max(-(-total // count), total * portions[0] // sum(portions)))
    least = 1 if total - largest >= count - 1 else 0
    given, surplus = [largest] + [least] * (count - 1), total - largest - least * (count - 1)
    while surplus > 0:
        movable = [i for i in range(1, count) if given[i] < largest] or [i for i in range(1, count) if given[i] < most]
        pool, budget = sum([portions[i] for i in movable]), surplus
        for i in movable:
            more = min(most - given[i], max(1, budget * portions[i] // pool), surplus)
            given[i] = given[i] + more
            surplus = surplus - more
    return np.array(given)


def normal_values(key, shape, spread, reach, shards=(), held_as=jnp.bfloat16):
    entries = jax.random.normal(key, shape, jnp.float32) * spread
    if len(shards) > 0:
        entries = levels(key, shape, shards, -0.22, 0.18) * entries
    return jnp.clip(entries, min=-reach, max=reach).astype(held_as)


def setup_inputs(seed: int = 0) -> dict:
    splits = jax.random.split(jax.random.key(seed), 17)
    query_one = draw_query_one(jax.random.fold_in(splits[16], 71), 0)
    key_one = draw_key_one(jax.random.fold_in(splits[16], 71), 0)
    query_two = draw_query_two(jax.random.fold_in(splits[16], 71), 0)
    key_two = draw_key_two(jax.random.fold_in(splits[16], 71), 0)
    values = normal_values(splits[4], (TOKENS, MIXW), 1.0, 6.0, ((0, 8), (1, 4)))
    mix_lambda = jnp.clip(0.3 + 0.5 * jax.random.uniform(splits[5], (HEADS,), jnp.float32) ** levels(splits[5], (HEADS,), ((0, 4),), -0.2, 0.2), 0.3, 0.8)
    head_gain = jnp.clip(1.0 + 0.18 * jax.random.normal(splits[6], (VD,), jnp.float32), 0.1, 1.9)
    residual_in = normal_values(splits[7], (TOKENS, D), 1.0, 6.0, ((0, 32),))
    out_weight = normal_values(splits[8], (MIXW, D), MIXW ** -0.5, 0.1875)
    norm_gain = jnp.clip(1.0 + 0.18 * jax.random.normal(splits[9], (D,), jnp.float32), 0.1, 1.9)
    route_ids_keys = jax.random.split(jax.random.fold_in(splits[10], 1), TOKENS // ROWS)
    route_ids_turns = jax.random.permutation(jax.random.fold_in(splits[10], 3), TOKENS // ROWS)
    route_ids = jax.vmap(lambda own, number: deal_out(jax.random.fold_in(splits[10], 2), own, number, ROWS, EXPERTS, TOP, CAP, 2))(route_ids_keys, route_ids_turns).reshape((TOKENS, TOP))
    route_logits = normal_values(splits[11], (TOKENS, TOP), 1.0, 6.0, ((0, 32),), jnp.float32)
    group_prob = jnp.clip(0.25 + 0.75 * jax.random.uniform(splits[12], (TOKENS,), jnp.float32) ** levels(splits[12], (TOKENS,), ((0, 32),), -0.2, 0.2), 0.25, 1.0)
    gate_weight = normal_values(splits[13], (EXPERTS, D, FF), D ** -0.5, 0.125, ((0, 8), (2, 4)))
    up_weight = normal_values(splits[14], (EXPERTS, D, FF), D ** -0.5, 0.125, ((0, 8), (2, 4)))
    down_weight = normal_values(splits[15], (EXPERTS, FF, D), FF ** -0.5, 0.1875, ((0, 8), (1, 4)))
    return {"query_one": query_one, "key_one": key_one, "query_two": query_two, "key_two": key_two, "values": values, "mix_lambda": mix_lambda, "head_gain": head_gain, "residual_in": residual_in, "out_weight": out_weight, "norm_gain": norm_gain, "route_ids": route_ids, "route_logits": route_logits, "group_prob": group_prob, "gate_weight": gate_weight, "up_weight": up_weight, "down_weight": down_weight}


norm_epsilon = 1e-06

def round_kept(value):
    return lax.optimization_barrier(value.astype(jnp.bfloat16)).astype(jnp.float32)

def head_output(query_a, key_a, query_b, key_b, head_values, weight_two, gain):
    score_scale = 1.0 / math.sqrt(QK)
    block_rows = min(512, TOKENS)

    def one_map(queries, keys):
        scores = jnp.dot(queries, keys.T, preferred_element_type=jnp.float32) * score_scale
        top_score = lax.optimization_barrier(jnp.max(scores, axis=-1, keepdims=True))
        expo = jnp.exp(scores - top_score)
        summed = lax.optimization_barrier(jnp.sum(expo, axis=-1, keepdims=True))
        return jnp.dot(expo.astype(jnp.bfloat16), head_values, preferred_element_type=jnp.float32) / summed

    def one_block(pair):
        block_a, block_b = pair
        combined = one_map(block_a, key_a) - weight_two * one_map(block_b, key_b)
        combined = combined * lax.rsqrt(lax.optimization_barrier(jnp.mean(combined * combined, axis=-1, keepdims=True)) + norm_epsilon) * gain
        return combined.astype(jnp.bfloat16)
    blocks = lax.map(one_block, (query_a.reshape(TOKENS // block_rows, block_rows, QK), query_b.reshape(TOKENS // block_rows, block_rows, QK)))
    return blocks.reshape(TOKENS, VD)

def reference(query_one, key_one, query_two, key_two, values, mix_lambda, head_gain, residual_in, out_weight, norm_gain, route_ids, route_logits, group_prob, gate_weight, up_weight, down_weight):

    def by_head(array, size):
        return array.reshape(TOKENS, HEADS, size).transpose(1, 0, 2)

    def run_head(packed):
        qa, ka, qb, kb, vals, weight_two = packed
        return head_output(qa, ka, qb, kb, vals, weight_two, head_gain)
    heads_out = lax.map(run_head, (by_head(query_one, QK), by_head(key_one, QK), by_head(query_two, QK), by_head(key_two, QK), by_head(values, VD), mix_lambda))
    attended = heads_out.transpose(1, 0, 2).reshape(TOKENS, MIXW)
    mix = jnp.dot(attended, out_weight, preferred_element_type=jnp.float32)
    hidden = (residual_in.astype(jnp.float32) + mix).astype(jnp.bfloat16)
    hidden_f = hidden.astype(jnp.float32)
    normed = (hidden_f * lax.rsqrt(lax.optimization_barrier(jnp.mean(hidden_f * hidden_f, axis=-1, keepdims=True)) + norm_epsilon) * norm_gain).astype(jnp.bfloat16)
    route_weight = jax.nn.softmax(route_logits, axis=-1) * group_prob[:, None]
    flat_ids = route_ids.reshape(-1)
    flat_weight = route_weight.reshape(-1)
    limit = CAP * N_SP * N_TP
    positions = jnp.arange(TOKENS * TOP, dtype=jnp.int32)
    block_ff = FF // N_TP

    def expert_step(running, expert):
        hit = flat_ids == expert
        rank = jnp.cumsum(hit.astype(jnp.int32)) - 1
        where_to = jnp.where(hit, rank, limit).astype(jnp.int32)
        chosen = jnp.zeros((limit,), jnp.int32).at[where_to].set(positions, mode='drop')
        live = jnp.zeros((limit,), jnp.float32).at[where_to].set(1.0, mode='drop')
        token_of = chosen // TOP
        picked = normed[token_of]
        gate = jnp.dot(picked, gate_weight[expert], preferred_element_type=jnp.float32)
        upper = jnp.dot(picked, up_weight[expert], preferred_element_type=jnp.float32)
        middle = (jax.nn.silu(gate) * upper).astype(jnp.bfloat16)
        down = down_weight[expert]
        summed = jnp.zeros((limit, D), jnp.float32)
        for piece in range(N_TP):
            part_sum = jnp.dot(middle[:, piece * block_ff:(piece + 1) * block_ff], down[piece * block_ff:(piece + 1) * block_ff], preferred_element_type=jnp.float32)
            summed = summed + round_kept(part_sum)
        expert_out = round_kept(summed)
        scaled = expert_out * (flat_weight[chosen] * live)[:, None]
        return (running.at[token_of].add(scaled), None)
    moe, _ = lax.scan(expert_step, jnp.zeros((TOKENS, D), jnp.float32), jnp.arange(EXPERTS, dtype=jnp.int32))
    return (hidden_f + moe).astype(jnp.bfloat16)
```

```python
import functools
import math

import jax
import jax.numpy as jnp
from jax import lax
from jax.experimental import pallas as pl
from jax.experimental.pallas import tpu as pltpu
from jax.sharding import PartitionSpec as P

norm_epsilon = 1e-06
VMEM = pltpu.VMEM
PERMUTE_LIMIT = 8


def vspec():
    return pl.BlockSpec(memory_space=VMEM)


def xor_pairs(size, mask):
    return [(i, i ^ mask) for i in range(size)]


def log2(n):
    assert n > 0 and n & (n - 1) == 0
    return n.bit_length() - 1


def params(mib):
    return pltpu.CompilerParams(vmem_limit_bytes=mib * 1024 * 1024)


def attention_kernel(geo, tok_ref, qa_ref, qb_ref, lam_ref, gain_ref, *refs):
    heads, qk, vd, share, le, ts, n_kv = geo
    kv = refs[:n_kv]
    outs = refs[n_kv : n_kv + ts]
    qs_ref, s_ref = refs[n_kv + ts :]
    width = heads * qk
    rows = share * le * ts
    factor = math.log2(math.e) / math.sqrt(qk)
    for q in range(ts):
        for j in range(le):
            at = pl.multiple_of(tok_ref[j * ts + q] * share, share)
            here = (q * le + j) * share
            qs_ref[0, here : here + share, :] = qa_ref[pl.ds(at, share), :]
            qs_ref[1, here : here + share, :] = qb_ref[pl.ds(at, share), :]
    span = 256
    lane_head = lax.broadcasted_iota(jnp.int32, (rows, width), 1) // qk

    def one_map(m, h):
        query = jnp.where(lane_head == h, qs_ref[m], jnp.zeros((), jnp.bfloat16))

        def score(ref, at, col, top):
            keys = ref[pl.ds(at, span), m * width : (m + 1) * width]
            s = lax.dot_general(
                query, keys, (((1,), (1,)), ((), ())), preferred_element_type=jnp.float32
            )
            s_ref[:, pl.ds(col, span)] = s
            for c in range(span // 128):
                top = jnp.maximum(top, s[:, c * 128 : (c + 1) * 128])
            return top

        def weigh(ref, at, col, high, state):
            total, acc = state
            p = jnp.exp2((s_ref[:, pl.ds(col, span)] - high) * factor)
            for c in range(span // 128):
                total = total + p[:, c * 128 : (c + 1) * 128]
            lo = 2 * width + h * vd
            vals = ref[pl.ds(at, span), lo : lo + vd]
            acc = acc + jnp.dot(
                p.astype(jnp.bfloat16), vals, preferred_element_type=jnp.float32
            )
            return total, acc

        def sweep(step, state):
            col = 0
            for ref in kv:
                count = ref.shape[0] // span
                if count == 1:
                    state = step(ref, 0, col, state)
                else:
                    state = lax.fori_loop(
                        0,
                        count,
                        lambda i, st, ref=ref, col=col: step(
                            ref,
                            pl.multiple_of(i * span, span),
                            pl.multiple_of(col + i * span, span),
                            st,
                        ),
                        state,
                    )
                col += count * span
            return state

        top = sweep(score, jnp.full((rows, 128), -jnp.inf, jnp.float32))
        high = jnp.max(top, axis=-1, keepdims=True)
        total, acc = sweep(
            lambda ref, at, col, st: weigh(ref, at, col, high, st),
            (jnp.zeros((rows, 128), jnp.float32), jnp.zeros((rows, vd), jnp.float32)),
        )
        return acc / jnp.sum(total, axis=-1, keepdims=True)

    for h in range(heads):
        read = one_map(0, h) - lam_ref[h] * one_map(1, h)
        scale = lax.rsqrt(jnp.mean(read * read, axis=-1, keepdims=True) + norm_epsilon)
        done = (read * scale * gain_ref[...]).astype(jnp.bfloat16)
        for q in range(ts):
            outs[q][:, h * vd : (h + 1) * vd] = done[q * le * share : (q + 1) * le * share]


def table_kernel(geo, meta_ref, expert_ref, table_ref, *back):
    n_sp, le, cap, share = geo
    tokens = le * share
    first, second = meta_ref[0:1, :], meta_ref[1:2, :]
    expert = expert_ref[...]
    hit_a, hit_b = first == expert, second == expert
    hit = jnp.where(hit_a | hit_b, 1.0, 0.0)
    weight = jnp.where(hit_a, meta_ref[2:3, :], 0.0) + jnp.where(hit_b, meta_ref[3:4, :], 0.0)
    before = lax.broadcasted_iota(jnp.int32, (tokens, tokens), 0)
    after = lax.broadcasted_iota(jnp.int32, (tokens, tokens), 1)
    same = (before >> log2(share)) == (after >> log2(share))
    order = jnp.where(same & (before < after), 1.0, 0.0).astype(jnp.bfloat16)
    dot = functools.partial(jnp.dot, preferred_element_type=jnp.float32)
    hit = hit.astype(jnp.bfloat16)
    rank = dot(hit, order).astype(jnp.bfloat16)
    high = weight.astype(jnp.bfloat16)
    low = (weight - high.astype(jnp.float32)).astype(jnp.bfloat16)

    def spread(slots, per):
        s = lax.broadcasted_iota(jnp.int32, (slots, n_sp), 0)
        p = lax.broadcasted_iota(jnp.int32, (slots, n_sp), 1)
        return jnp.where((s >> log2(per)) == p, 1.0, 0.0).astype(jnp.bfloat16)

    def chosen(expand, slots):
        s = lax.broadcasted_iota(jnp.int32, (slots, tokens), 0)
        place = (s & (cap - 1)).astype(jnp.float32)
        return (dot(expand, hit) > 0.5) & (dot(expand, rank) == place), s

    slots = n_sp * le * cap
    token_set = lax.broadcasted_iota(jnp.int32, (slots, tokens), 1) >> log2(share)
    mask, s = chosen(spread(slots, le * cap), slots)
    mask = mask & (((s >> log2(cap)) & (le - 1)) == token_set)
    table_ref[...] = jnp.where(mask, 1.0, 0.0).astype(jnp.bfloat16)
    slots = n_sp * cap
    expand = spread(slots, cap)
    mask, _ = chosen(expand, slots)
    for part, out in ((high, back[0]), (low, back[1])):
        placed = jnp.where(mask, dot(expand, part), 0.0)
        out[...] = placed.T.astype(jnp.bfloat16)


def post_kernel(geo, row_ref, gain_ref, table_ref, w_ref, *refs):
    tp, le, ts, share, n_out = geo
    att = refs[:tp]
    res = refs[tp : tp + le]
    hidden_ref = refs[tp + le]
    outs = refs[tp + le + 1 : tp + le + 1 + n_out]
    (keep_ref,) = refs[tp + le + 1 + n_out :]
    tokens, width = keep_ref.shape
    depth = att[0].shape[1]
    pieces = []
    for k in range(tp):
        swap = k // ts
        pieces.append(
            jnp.concatenate(
                [att[k][(j ^ swap) * share : ((j ^ swap) + 1) * share, :] for j in range(le)], axis=0
            )
        )
    tile = 512
    squares = jnp.zeros((tokens, 128), jnp.float32)
    for n in range(width // tile):
        cols = slice(n * tile, (n + 1) * tile)
        mix = jnp.zeros((tokens, tile), jnp.float32)
        for k in range(tp):
            at = pl.multiple_of(row_ref[k] * depth, depth)
            mix = mix + jnp.dot(
                pieces[k], w_ref[pl.ds(at, depth), cols], preferred_element_type=jnp.float32
            )
        base = jnp.concatenate([r[:, cols] for r in res], axis=0).astype(jnp.float32)
        kept = (base + mix).astype(jnp.bfloat16)
        keep_ref[:, cols] = kept
        kept = kept.astype(jnp.float32)
        kept = kept * kept
        for c in range(tile // 128):
            squares = squares + kept[:, c * 128 : (c + 1) * 128]
    scale = lax.rsqrt(jnp.sum(squares, axis=-1, keepdims=True) / width + norm_epsilon)
    hidden_ref[...] = keep_ref[0:share, :]
    per = table_ref.shape[0] // n_out
    for n in range(width // tile):
        cols = slice(n * tile, (n + 1) * tile)
        normed = (keep_ref[:, cols].astype(jnp.float32) * scale * gain_ref[:, cols]).astype(
            jnp.bfloat16
        )
        rows = jnp.dot(table_ref[...], normed, preferred_element_type=jnp.float32).astype(
            jnp.bfloat16
        )
        for k in range(n_out):
            outs[k][:, cols] = rows[k * per : (k + 1) * per, :]


def expert_kernel(geo, *refs):
    n_in, le, cap, n_piece, chunks, n_out = geo
    xs = refs[:n_in]
    at = n_in
    weights = []
    for count in chunks:
        weights.append([refs[at + i * count : at + (i + 1) * count] for i in range(n_piece)])
        at += n_piece * count
    outs = refs[at : at + n_out]
    x_ref, gate_ref, up_ref, down_ref, mid_ref, sems = refs[at + n_out :]
    held = (gate_ref, up_ref, down_ref)
    copies = [[[] for _ in range(n_piece)] for _ in range(3)]
    sem = 0
    order = [(w, i) for i in range(n_piece) for w in (0, 1)] + [(2, i) for i in range(n_piece)]
    for w, i in order:
        start = 0
        for chunk in weights[w][i]:
            rows = chunk.shape[0]
            copy = pltpu.make_async_copy(
                chunk, held[w].at[i, pl.ds(start, rows), :], sems.at[sem]
            )
            copy.start()
            copies[w][i].append(copy)
            start += rows
            sem += 1
    total = x_ref.shape[0]
    if n_in > 1:
        for j in range(le):
            for k in range(n_in):
                here = (j * n_in + k) * cap
                x_ref[here : here + cap, :] = xs[k][j * cap : (j + 1) * cap, :]
    else:
        x_ref[...] = xs[0][...]
    block = gate_ref.shape[2]
    for i in range(n_piece):
        for copy in copies[0][i] + copies[1][i]:
            copy.wait()
        gate = jnp.dot(x_ref[...], gate_ref[i], preferred_element_type=jnp.float32)
        upper = jnp.dot(x_ref[...], up_ref[i], preferred_element_type=jnp.float32)
        mid_ref[:, i * block : (i + 1) * block] = (gate / (1.0 + jnp.exp(-gate)) * upper).astype(
            jnp.bfloat16
        )
    for i in range(n_piece):
        for copy in copies[2][i]:
            copy.wait()
    width = down_ref.shape[2]
    tile = 512
    per = outs[0].shape[0]
    for n in range(width // tile):
        cols = slice(n * tile, (n + 1) * tile)
        acc = jnp.zeros((total, tile), jnp.float32)
        for i in range(n_piece):
            acc = acc + jnp.dot(
                mid_ref[:, i * block : (i + 1) * block],
                down_ref[i, :, cols],
                preferred_element_type=jnp.float32,
            )
        acc = acc.astype(jnp.bfloat16)
        for k in range(n_out):
            outs[k][:, cols] = acc[k * per : (k + 1) * per, :]


def combine_kernel(n_rows, n_add, high_ref, low_ref, *refs):
    rows = refs[:n_rows]
    adds = refs[n_rows : n_rows + n_add]
    out_ref = refs[n_rows + n_add]
    width = out_ref.shape[1]
    tile = 512
    for n in range(width // tile):
        cols = slice(n * tile, (n + 1) * tile)
        got = [r[:, cols] for r in rows]
        got = jnp.concatenate(got, axis=0) if n_rows > 1 else got[0]
        moe = jnp.dot(high_ref[...], got, preferred_element_type=jnp.float32)
        moe = moe + jnp.dot(low_ref[...], got, preferred_element_type=jnp.float32)
        for a in adds:
            moe = moe + a[:, cols].astype(jnp.float32)
        out_ref[:, cols] = moe.astype(jnp.bfloat16)


def on_device(
    query_one,
    key_one,
    query_two,
    key_two,
    values,
    mix_lambda,
    head_gain,
    residual_in,
    out_weight,
    norm_gain,
    route_ids,
    route_logits,
    group_prob,
    gate_weight,
    up_weight,
    down_weight,
):
    n_sp, tp = lax.axis_size("sp"), lax.axis_size("tp")
    row_count = query_one.shape[0]
    heads = mix_lambda.shape[0]
    qk = query_one.shape[1] // heads
    vd = values.shape[1] // heads
    share, width = residual_in.shape
    top = route_ids.shape[1]
    le = gate_weight.shape[0]
    ts = tp // le
    expert_count = le * n_sp
    cap = max(2, 2 * share * top // expert_count)
    assert top == 2 and ts * le == tp and share * tp == row_count
    for n in (n_sp, tp, le, ts, cap, share):
        log2(n)
    direct = n_sp <= PERMUTE_LIMIT
    t = lax.axis_index("tp")
    sp = lax.axis_index("sp")
    g = t // ts
    partners = jnp.stack([t ^ k for k in range(tp)]).astype(jnp.int32)

    def send(x, axis, mask):
        return lax.ppermute(x, axis, xor_pairs(lax.axis_size(axis), mask))

    packed = jnp.concatenate([key_one, key_two, values], axis=1)
    if direct:
        far = [send(packed, "sp", k) for k in range(n_sp - 2, 0, -2)]
        near = [send(packed, "sp", 1)] if n_sp > 1 else []
        kv = [packed] + near + far + [send(b, "sp", 1) for b in far]
    else:
        kv = [lax.all_gather(packed, "sp", axis=0, tiled=True)]

    route_weight = jax.nn.softmax(route_logits, axis=-1) * group_prob[:, None]
    meta = jnp.concatenate(
        [route_ids.astype(jnp.float32).T, route_weight.T, jnp.zeros((4, share), jnp.float32)], axis=0
    )
    metas = [meta] + [send(meta, "tp", j * ts) for j in range(1, le)]
    residuals = [residual_in] + [send(residual_in, "tp", j * ts) for j in range(1, le)]

    def block_of(w, which):
        return lax.dynamic_index_in_dim(w, which, axis=0, keepdims=False)

    def gather_weight(w, parts, late):
        own = block_of(w, g)
        rows = own.shape[0] // len(parts)
        held = [[own[p * rows : (p + 1) * rows] for p in range(len(parts))]]
        for j in range(1, le):
            away = block_of(w, g ^ j)
            got = []
            for p, is_late in enumerate(parts):
                x = away[p * rows : (p + 1) * rows]
                if is_late:
                    x, _ = lax.optimization_barrier((x, late))
                got.append(send(x, "tp", j * ts))
            held.append(got)
        out = list(held)
        for q in range(1, ts):
            for pieces in held:
                out.append([send(x, "tp", q) for x in pieces])
        return out

    attended = pl.pallas_call(
        functools.partial(
            attention_kernel, (heads, qk, vd, share, le, ts, len(kv))
        ),
        out_shape=[jax.ShapeDtypeStruct((le * share, heads * vd), jnp.bfloat16)] * ts,
        in_specs=[pl.BlockSpec(memory_space=pltpu.SMEM), vspec(), vspec()]
        + [pl.BlockSpec(memory_space=pltpu.SMEM), vspec()]
        + [vspec()] * len(kv),
        out_specs=[vspec()] * ts,
        scratch_shapes=[
            VMEM((2, row_count, heads * qk), jnp.bfloat16),
            VMEM((row_count, row_count * n_sp), jnp.float32),
        ],
        compiler_params=params(48 if not direct else 16),
        cost_estimate=pl.CostEstimate(
            flops=2_000_000_000, bytes_accessed=4_000_000, transcendentals=2_000_000
        ),
        name="attention",
    )(partners, query_one, query_two, mix_lambda, head_gain.reshape(1, vd), *kv)

    late = attended[0]
    gates = gather_weight(gate_weight, (False,), late)
    ups = gather_weight(up_weight, (False, True), late)
    downs = gather_weight(down_weight, (True,), late)

    gathered = [attended[0]] + [send(attended[k % ts], "tp", k) for k in range(1, tp)]

    places = jnp.arange(n_sp, dtype=jnp.int32)
    experts = ((places ^ sp) if direct else places) * le + g
    slots = n_sp * le * cap
    table, high, low = pl.pallas_call(
        functools.partial(table_kernel, (n_sp, le, cap, share)),
        out_shape=[
            jax.ShapeDtypeStruct((slots, le * share), jnp.bfloat16),
            jax.ShapeDtypeStruct((le * share, n_sp * cap), jnp.bfloat16),
            jax.ShapeDtypeStruct((le * share, n_sp * cap), jnp.bfloat16),
        ],
        in_specs=[vspec()] * 2,
        out_specs=[vspec()] * 3,
        compiler_params=params(4),
        name="tables",
    )(jnp.concatenate(metas, axis=1), experts.astype(jnp.float32).reshape(n_sp, 1))

    n_out = n_sp if direct else 1
    hidden, *outgoing = pl.pallas_call(
        functools.partial(post_kernel, (tp, le, ts, share, n_out)),
        out_shape=[jax.ShapeDtypeStruct((share, width), jnp.bfloat16)]
        + [jax.ShapeDtypeStruct((slots // n_out, width), jnp.bfloat16)] * n_out,
        in_specs=[pl.BlockSpec(memory_space=pltpu.SMEM)] + [vspec()] * (3 + tp + le),
        out_specs=[vspec()] * (1 + n_out),
        scratch_shapes=[VMEM((le * share, width), jnp.bfloat16)],
        compiler_params=params(16),
        cost_estimate=pl.CostEstimate(
            flops=2_000_000_000, bytes_accessed=6_000_000, transcendentals=0
        ),
        name="project",
    )(partners, norm_gain.reshape(1, width), table, out_weight, *gathered, *residuals)

    if direct:
        arrived = [outgoing[0]] + [None] * (n_sp - 1)
        for k in range(n_sp - 1, 0, -1):
            arrived[k] = send(outgoing[k], "sp", k)
    else:
        got = lax.all_to_all(outgoing[0], "sp", split_axis=0, concat_axis=0, tiled=True)
        got = got.reshape(n_sp, le, cap, width).transpose(1, 0, 2, 3)
        arrived = [got.reshape(slots, width)]

    hbm = pl.BlockSpec(memory_space=pltpu.HBM)
    groups = (gates, ups, downs)
    chunks = tuple(len(group[0]) for group in groups)
    flat = [x for group in groups for piece in group for x in piece]
    block = gate_weight.shape[2]
    n_ret = le * n_sp if direct else le
    answers = pl.pallas_call(
        functools.partial(expert_kernel, (len(arrived), le, cap, tp, chunks, n_ret)),
        out_shape=[jax.ShapeDtypeStruct((slots // n_ret, width), jnp.bfloat16)] * n_ret,
        in_specs=[vspec()] * len(arrived) + [hbm] * len(flat),
        out_specs=[vspec()] * n_ret,
        scratch_shapes=[
            VMEM((slots, width), jnp.bfloat16),
            VMEM((tp, width, block), jnp.bfloat16),
            VMEM((tp, width, block), jnp.bfloat16),
            VMEM((tp, block, width), jnp.bfloat16),
            VMEM((slots, tp * block), jnp.bfloat16),
            pltpu.SemaphoreType.DMA((len(flat),)),
        ],
        compiler_params=params(28),
        cost_estimate=pl.CostEstimate(
            flops=3_200_000_000, bytes_accessed=14_000_000, transcendentals=300_000
        ),
        name="experts",
    )(*arrived, *flat)

    def fetch(j):
        if not direct:
            return [lax.all_to_all(answers[j], "sp", split_axis=0, concat_axis=0, tiled=True)]
        mine = answers[j * n_sp : (j + 1) * n_sp]
        back = [mine[0]] + [None] * (n_sp - 1)
        for k in range(n_sp - 1, 0, -1):
            back[k] = send(mine[k], "sp", k)
        return back

    def combine(j, rows, adds):
        part = slice(j * share, (j + 1) * share)
        return pl.pallas_call(
            functools.partial(combine_kernel, len(rows), len(adds)),
            out_shape=jax.ShapeDtypeStruct((share, width), jnp.bfloat16),
            in_specs=[vspec()] * (2 + len(rows) + len(adds)),
            out_specs=vspec(),
            compiler_params=params(8),
            cost_estimate=pl.CostEstimate(
                flops=70_000_000, bytes_accessed=1_000_000, transcendentals=0
            ),
            name="combine",
        )(high[part], low[part], *rows, *adds)

    extra = [send(combine(j, fetch(j), []), "tp", j * ts) for j in range(1, le)]
    return combine(0, fetch(0), [hidden] + extra)


def solution(mesh):
    in_specs = (
        P("sp", "tp"),
        P("sp", "tp"),
        P("sp", "tp"),
        P("sp", "tp"),
        P("sp", "tp"),
        P("tp"),
        P(),
        P(("sp", "tp"), None),
        P(),
        P(),
        P(("sp", "tp"), None),
        P(("sp", "tp"), None),
        P(("sp", "tp")),
        P("sp", None, "tp"),
        P("sp", None, "tp"),
        P("sp", "tp", None),
    )
    out_specs = P(("sp", "tp"), None)
    return jax.shard_map(
        on_device, mesh=mesh, in_specs=in_specs, out_specs=out_specs, check_vma=False
    )
```
